32 devices in a mesh: sp: 4 (over y, x), dp: 8 (over z, core).
Axes of the slice: x: 2, y: 2, z: 4, core: 2. Of those that a mesh axis runs over, the one named last changes fastest.
Arguments:
- tokens: bfloat16 [8, 640, 2048], P('dp', 'sp'), may hold values from -42 to 42
- query_weight: bfloat16 [2048, 1024], P('dp'), may hold values from -1 to 1
- key_weight: bfloat16 [2048, 1024], P('dp'), may hold values from -1 to 1
- values: bfloat16 [8, 640, 1024], P('dp', 'sp'), may hold values from -6 to 6
- lambdas: float32 [16], replicated, may hold values from 0.3 to 0.8
- out_grad: bfloat16 [8, 640, 1024], P('dp', 'sp'), may hold values from -6 to 6
Outputs:
- tokens_grad: bfloat16 [8, 640, 2048], P('dp', 'sp')
- values_grad: bfloat16 [8, 640, 1024], P('dp', 'sp')
- query_weight_grad: float32 [2048, 1024], P('dp')
- key_weight_grad: float32 [2048, 1024], P('dp')
The draws below stay inside these ranges and needn't reach their ends.
All inputs are finite; a program needn't handle non-finite values.
Results may differ from the reference program's by a relative error of at most 0.029.
The reference program's roundings to bfloat16 on the way count: a program that leaves them out, or rounds other values in their place, can miss the bound.
Values may be sent and summed in bfloat16 or wider, within the bound.
No kernel may reach another device: no remote copies, remote signals or barrier semaphores. Data moves between devices by JAX's collectives and lax.ppermute only.
A program may use at most 128 MiB of HBM per device.

```python
import math
import jax
import jax.numpy as jnp
from jax import lax

D = 2048
HEADS = 16
DQK = 32
SEQLEN = 640
BATCH = 8
QCOLS = 1024
VCOLS = 1024


def weight_normals(key):
    first_draw = jax.random.normal(jax.random.fold_in(key, 11), (D, QCOLS), jnp.float32)
    second_draw = jax.random.normal(jax.random.fold_in(key, 12), (D, QCOLS), jnp.float32)
    return (first_draw, second_draw)


def draw_query_weight(key, part):
    first_draw, second_draw = weight_normals(key)
    return (jnp.clip(first_draw, -6.0, 6.0) * math.sqrt(3.0 / D)).astype(jnp.bfloat16)


def draw_key_weight(key, part):
    first_draw, second_draw = weight_normals(key)
    blended = second_draw
    return (jnp.clip(blended, -6.0, 6.0) * math.sqrt(1.0 / D)).astype(jnp.bfloat16)


def draw_tokens(key, part):
    base_draw = jnp.clip(jax.random.normal(jax.random.fold_in(key, 21), (BATCH, SEQLEN, D), jnp.float32), -6.0, 6.0)
    return base_draw.astype(jnp.bfloat16)


def levels(rng, dims, split, smallest, largest):
    factor_of, own = 1.0, jax.random.fold_in(rng, 6)
    for dim, shards_of in split:
        draws = jnp.exp(jax.random.uniform(jax.random.fold_in(own, dim), (shards_of,), jnp.float32, smallest / len(split), largest / len(split)))
        factor_of = factor_of * jnp.repeat(draws, dims[dim] // shards_of).reshape([-1 if axis == dim else 1 for axis in range(len(dims))])
    return factor_of


def gaussian(own_key, shape, scale, reach, pieces=(), kind=jnp.bfloat16):
    level = levels(own_key, shape, pieces, -0.22, 0.18) if pieces else 1.0
    entries = jax.random.normal(own_key, shape, jnp.float32) * scale * level
    return jnp.minimum(jnp.maximum(entries, -reach), reach).astype(kind)


def setup_inputs(seed: int = 0) -> dict:
    arg_keys = jax.random.split(jax.random.key(seed), 7)
    tokens = draw_tokens(jax.random.fold_in(arg_keys[6], 71), 0)
    query_weight = draw_query_weight(jax.random.fold_in(arg_keys[6], 71), 0)
    key_weight = draw_key_weight(jax.random.fold_in(arg_keys[6], 71), 0)
    values = gaussian(arg_keys[3], (BATCH, SEQLEN, VCOLS), 1.0, 6.0, ((0, 8), (1, 4)))
    lambdas = jnp.clip(jax.random.uniform(arg_keys[4], (HEADS,), jnp.float32, 0.3, 0.8), 0.3, 0.8)
    out_grad = gaussian(arg_keys[5], (BATCH, SEQLEN, VCOLS), 1.0, 6.0, ((0, 8), (1, 4)))
    return dict(tokens=tokens, query_weight=query_weight, key_weight=key_weight, values=values, lambdas=lambdas, out_grad=out_grad)


NORM_EPS = 0.1
THETA = 10000.0

def rotation_tables(positions, vec_width):
    half_width = vec_width // 2
    freqs = jnp.exp(-math.log(THETA) * jnp.arange(half_width, dtype=jnp.float32) / half_width)
    angles = positions.astype(jnp.float32)[:, None] * freqs[None, :]
    return (jnp.cos(angles), jnp.sin(angles))

def rotate(field, cosine, sine_table, vec_width, sign_value):
    full_shape = field.shape
    grouped = field.reshape(full_shape[:-1] + (full_shape[-1] // vec_width, 2, vec_width // 2))
    first_half = grouped[..., 0, :]
    second_half = grouped[..., 1, :]
    cos_cols = cosine[:, None, :]
    sin_cols = sign_value * sine_table[:, None, :]
    turned = jnp.stack([first_half * cos_cols - second_half * sin_cols, second_half * cos_cols + first_half * sin_cols], axis=-2)
    return turned.reshape(full_shape)

def pair_product(pattern, first_op, second_op):
    return jnp.einsum(pattern, first_op.astype(jnp.float32), second_op.astype(jnp.float32))

def head_backward(query_rot, key_rot, value_rows, grad_rows, lambda_here, cosine, sine_table):
    seq_length = query_rot.shape[0]
    head_count = lambda_here.shape[0]
    qk_width = query_rot.shape[1] // (2 * head_count)
    value_width = value_rows.shape[1] // head_count
    block_rows = math.gcd(seq_length, 512)
    block_count = seq_length // block_rows
    inv_root = 1.0 / math.sqrt(qk_width)
    query_split = query_rot.reshape(block_count, block_rows, head_count, 2, qk_width)
    key_split = key_rot.reshape(seq_length, head_count, 2, qk_width)
    value_split = value_rows.reshape(seq_length, head_count, value_width)
    grad_split = grad_rows.reshape(block_count, block_rows, head_count, value_width)
    lambda_col = lambda_here[:, None, None]
    key_positions = jnp.arange(seq_length, dtype=jnp.int32)

    def block_step(carried, inputs):
        key_sum, value_sum = carried
        query_part, grad_part, block_start = inputs
        scores = pair_product('qhmd,khmd->hmqk', query_part, key_split) * inv_root
        query_positions = block_start + jnp.arange(block_rows, dtype=jnp.int32)
        causal_mask = key_positions[None, :] <= query_positions[:, None]
        scores = jnp.where(causal_mask, scores, -jnp.inf)
        row_max = lax.optimization_barrier(jnp.max(scores, axis=-1, keepdims=True))
        exp_scores = jnp.exp(scores - row_max)
        prob_maps = exp_scores / lax.optimization_barrier(jnp.sum(exp_scores, axis=-1, keepdims=True))
        weights = (prob_maps[:, 0] - lambda_col * prob_maps[:, 1]).astype(jnp.bfloat16)
        mixed_out = pair_product('hqk,khe->qhe', weights, value_split)
        norm_scale = lax.rsqrt(lax.optimization_barrier(jnp.mean(mixed_out * mixed_out, axis=-1, keepdims=True)) + NORM_EPS)
        grad_float = grad_part.astype(jnp.float32)
        mixed_grad = (norm_scale * grad_float - norm_scale * norm_scale * norm_scale * mixed_out * lax.optimization_barrier(jnp.mean(grad_float * mixed_out, axis=-1, keepdims=True))).astype(jnp.bfloat16)
        weight_grad = pair_product('qhe,khe->hqk', mixed_grad, value_split)
        value_sum = value_sum + pair_product('hqk,qhe->khe', weights, mixed_grad)
        first_grad = prob_maps[:, 0] * (weight_grad - lax.optimization_barrier(jnp.sum(weight_grad * prob_maps[:, 0], axis=-1, keepdims=True)))
        second_grad = -lambda_col * prob_maps[:, 1] * (weight_grad - lax.optimization_barrier(jnp.sum(weight_grad * prob_maps[:, 1], axis=-1, keepdims=True)))
        score_grad = (jnp.stack([first_grad, second_grad], axis=1) * inv_root).astype(jnp.bfloat16)
        query_grad = pair_product('hmqk,khmd->qhmd', score_grad, key_split)
        key_sum = key_sum + pair_product('hmqk,qhmd->khmd', score_grad, query_part)
        return ((key_sum, value_sum), query_grad)
    zero_init = (jnp.zeros((seq_length, head_count, 2, qk_width), jnp.float32), jnp.zeros((seq_length, head_count, value_width), jnp.float32))
    block_starts = jnp.arange(block_count, dtype=jnp.int32) * block_rows
    (key_sum, value_sum), query_blocks = lax.scan(block_step, zero_init, (query_split, grad_split, block_starts))
    query_turned = query_blocks.reshape(seq_length, head_count * 2 * qk_width)
    key_turned = key_sum.reshape(seq_length, head_count * 2 * qk_width)
    query_back = rotate(query_turned, cosine, sine_table, qk_width, -1.0).astype(jnp.bfloat16)
    key_back = rotate(key_turned, cosine, sine_table, qk_width, -1.0).astype(jnp.bfloat16)
    values_back = value_sum.reshape(seq_length, head_count * value_width).astype(jnp.bfloat16)
    return (query_back, key_back, values_back)

def reference(tokens, query_weight, key_weight, values, lambdas, out_grad):
    cosine, sine_table = rotation_tables(jnp.arange(SEQLEN, dtype=jnp.int32), DQK)
    query_float = query_weight.astype(jnp.float32)
    key_float = key_weight.astype(jnp.float32)

    def one_sequence(inputs):
        token_seq, value_seq, grad_seq = inputs
        token_float = token_seq.astype(jnp.float32)
        query_rot = rotate(jnp.dot(token_float, query_float), cosine, sine_table, DQK, 1.0).astype(jnp.bfloat16)
        key_rot = rotate(jnp.dot(token_float, key_float), cosine, sine_table, DQK, 1.0).astype(jnp.bfloat16)
        query_back, key_back, values_back = head_backward(query_rot, key_rot, value_seq, grad_seq, lambdas, cosine, sine_table)
        query_back_f = query_back.astype(jnp.float32)
        key_back_f = key_back.astype(jnp.float32)
        input_grad = (jnp.dot(query_back_f, query_float.T) + jnp.dot(key_back_f, key_float.T)).astype(jnp.bfloat16)
        query_part = jnp.dot(token_float.T, query_back_f)
        key_part = jnp.dot(token_float.T, key_back_f)
        return (input_grad, values_back, query_part, key_part)
    tokens_grad, values_grad, query_parts, key_parts = lax.map(one_sequence, (tokens, values, out_grad))
    factor = 1.0 / math.sqrt(BATCH * SEQLEN)
    return (tokens_grad, values_grad, lax.optimization_barrier(jnp.sum(query_parts, axis=0)) * factor, lax.optimization_barrier(jnp.sum(key_parts, axis=0)) * factor)
```

```python
import functools
import math

import jax
import jax.numpy as jnp
from jax import lax
from jax.experimental import pallas as pl
from jax.experimental.pallas import tpu as pltpu
from jax.sharding import PartitionSpec as P

DQK = 32


NORM_EPS = 0.1
THETA = 10000.0


def rotation_tables(positions, vec_width):
    half_width = vec_width // 2
    freqs = jnp.exp(-math.log(THETA) * jnp.arange(half_width, dtype=jnp.float32) / half_width)
    angles = positions.astype(jnp.float32)[:, None] * freqs[None, :]
    return (jnp.cos(angles), jnp.sin(angles))


def rotate(field, cosine, sine_table, vec_width, sign_value):
    full_shape = field.shape
    grouped = field.reshape(full_shape[:-1] + (full_shape[-1] // vec_width, 2, vec_width // 2))
    first_half = grouped[..., 0, :]
    second_half = grouped[..., 1, :]
    cos_cols = cosine[:, None, :]
    sin_cols = sign_value * sine_table[:, None, :]
    turned = jnp.stack(
        [
            first_half * cos_cols - second_half * sin_cols,
            second_half * cos_cols + first_half * sin_cols,
        ],
        axis=-2,
    )
    return turned.reshape(full_shape)


def pair_product(pattern, first_op, second_op):
    return jnp.einsum(pattern, first_op, second_op, preferred_element_type=jnp.float32)


def head_backward(query_rot, key_rot, value_rows, grad_rows, lambda_here, cosine, sine_table):
    seq_length = query_rot.shape[0]
    head_count = lambda_here.shape[0]
    qk_width = query_rot.shape[1] // (2 * head_count)
    value_width = value_rows.shape[1] // head_count
    block_rows = math.gcd(seq_length, 512)
    block_count = seq_length // block_rows
    inv_root = 1.0 / math.sqrt(qk_width)
    query_split = query_rot.reshape(block_count, block_rows, head_count, 2, qk_width)
    key_split = key_rot.reshape(seq_length, head_count, 2, qk_width)
    value_split = value_rows.reshape(seq_length, head_count, value_width)
    grad_split = grad_rows.reshape(block_count, block_rows, head_count, value_width)
    lambda_col = lambda_here[:, None, None]
    key_positions = jnp.arange(seq_length, dtype=jnp.int32)

    def block_step(carried, inputs):
        key_sum, value_sum = carried
        query_part, grad_part, block_start = inputs
        scores = pair_product("qhmd,khmd->hmqk", query_part, key_split) * inv_root
        query_positions = block_start + jnp.arange(block_rows, dtype=jnp.int32)
        causal_mask = key_positions[None, :] <= query_positions[:, None]
        scores = jnp.where(causal_mask, scores, -jnp.inf)
        row_max = jnp.max(scores, axis=-1, keepdims=True)
        exp_scores = jnp.exp(scores - row_max)
        prob_maps = exp_scores / jnp.sum(exp_scores, axis=-1, keepdims=True)
        weights = (prob_maps[:, 0] - lambda_col * prob_maps[:, 1]).astype(jnp.bfloat16)
        mixed_out = pair_product("hqk,khe->qhe", weights, value_split)
        norm_scale = lax.rsqrt(jnp.mean(mixed_out * mixed_out, axis=-1, keepdims=True) + NORM_EPS)
        grad_float = grad_part.astype(jnp.float32)
        mixed_grad = (
            norm_scale * grad_float
            - norm_scale
            * norm_scale
            * norm_scale
            * mixed_out
            * jnp.mean(grad_float * mixed_out, axis=-1, keepdims=True)
        ).astype(jnp.bfloat16)
        weight_grad = pair_product("qhe,khe->hqk", mixed_grad, value_split)
        value_sum = value_sum + pair_product("hqk,qhe->khe", weights, mixed_grad)
        first_grad = prob_maps[:, 0] * (
            weight_grad - jnp.sum(weight_grad * prob_maps[:, 0], axis=-1, keepdims=True)
        )
        second_grad = (
            -lambda_col
            * prob_maps[:, 1]
            * (weight_grad - jnp.sum(weight_grad * prob_maps[:, 1], axis=-1, keepdims=True))
        )
        score_grad = (jnp.stack([first_grad, second_grad], axis=1) * inv_root).astype(jnp.bfloat16)
        query_grad = pair_product("hmqk,khmd->qhmd", score_grad, key_split)
        key_sum = key_sum + pair_product("hmqk,qhmd->khmd", score_grad, query_part)
        return ((key_sum, value_sum), query_grad)

    zero_init = (
        jnp.zeros((seq_length, head_count, 2, qk_width), jnp.float32),
        jnp.zeros((seq_length, head_count, value_width), jnp.float32),
    )
    block_starts = jnp.arange(block_count, dtype=jnp.int32) * block_rows
    (key_sum, value_sum), query_blocks = lax.scan(
        block_step, zero_init, (query_split, grad_split, block_starts)
    )
    query_turned = query_blocks.reshape(seq_length, head_count * 2 * qk_width)
    key_turned = key_sum.reshape(seq_length, head_count * 2 * qk_width)
    query_back = rotate(query_turned, cosine, sine_table, qk_width, -1.0).astype(jnp.bfloat16)
    key_back = rotate(key_turned, cosine, sine_table, qk_width, -1.0).astype(jnp.bfloat16)
    values_back = value_sum.reshape(seq_length, head_count * value_width).astype(jnp.bfloat16)
    return (query_back, key_back, values_back)


def general_body(tokens, query_weight, key_weight, values, lambdas, out_grad):
    sp_count = lax.axis_size("sp")
    dp_count = lax.axis_size("dp")
    tok_rows = tokens.shape[1]
    head_total = lambdas.shape[0]
    token_block = tokens[0]
    positions = lax.axis_index("sp") * tok_rows + jnp.arange(tok_rows, dtype=jnp.int32)
    cosine, sine_table = rotation_tables(positions, DQK)
    whole_query, whole_key = (
        lax.all_gather(query_weight, "dp", axis=0, tiled=True),
        lax.all_gather(key_weight, "dp", axis=0, tiled=True),
    )
    query_raw = jnp.dot(token_block, whole_query, preferred_element_type=jnp.float32)
    key_raw = jnp.dot(token_block, whole_key, preferred_element_type=jnp.float32)
    query_rot = rotate(query_raw, cosine, sine_table, DQK, 1.0).reshape(
        tok_rows, head_total, 2 * DQK
    )
    key_rot = rotate(key_raw, cosine, sine_table, DQK, 1.0).reshape(tok_rows, head_total, 2 * DQK)
    packed = (
        jnp.stack((query_rot, key_rot), axis=2)
        .reshape(1, tok_rows, head_total * 4 * DQK)
        .astype(jnp.bfloat16)
    )
    packed_heads, values_heads, grad_heads = (
        lax.all_to_all(packed, "sp", split_axis=2, concat_axis=1, tiled=True),
        lax.all_to_all(values, "sp", split_axis=2, concat_axis=1, tiled=True),
        lax.all_to_all(out_grad, "sp", split_axis=2, concat_axis=1, tiled=True),
    )
    heads_here = head_total // sp_count
    lambda_here = lax.dynamic_slice_in_dim(lambdas, lax.axis_index("sp") * heads_here, heads_here)
    seq_length = tok_rows * sp_count
    cosine_all, sine_all = rotation_tables(jnp.arange(seq_length, dtype=jnp.int32), DQK)
    head_split = packed_heads[0].reshape(seq_length, heads_here, 2, 2 * DQK)
    query_heads = head_split[:, :, 0].reshape(seq_length, heads_here * 2 * DQK)
    key_heads = head_split[:, :, 1].reshape(seq_length, heads_here * 2 * DQK)
    query_back, key_back, values_back = head_backward(
        query_heads, key_heads, values_heads[0], grad_heads[0], lambda_here, cosine_all, sine_all
    )
    packed_back = jnp.stack(
        (
            query_back.reshape(seq_length, heads_here, 2 * DQK),
            key_back.reshape(seq_length, heads_here, 2 * DQK),
        ),
        axis=2,
    )
    packed_back = packed_back.reshape(1, seq_length, heads_here * 4 * DQK)
    packed_tokens, values_grad = (
        lax.all_to_all(packed_back, "sp", split_axis=1, concat_axis=2, tiled=True),
        lax.all_to_all(values_back[None], "sp", split_axis=1, concat_axis=2, tiled=True),
    )
    packed_rows = packed_tokens[0]
    back_split = packed_rows.reshape(tok_rows, head_total, 2, 2 * DQK)
    query_tok = back_split[:, :, 0].reshape(tok_rows, head_total * 2 * DQK)
    key_tok = back_split[:, :, 1].reshape(tok_rows, head_total * 2 * DQK)
    contract = (((1,), (1,)), ((), ()))
    tokens_grad = lax.dot_general(
        query_tok, whole_query, contract, preferred_element_type=jnp.float32
    ) + lax.dot_general(key_tok, whole_key, contract, preferred_element_type=jnp.float32)
    outer_rows = (((0,), (0,)), ((), ()))
    grad_shard = lax.psum_scatter(
        lax.dot_general(
            token_block, packed_rows, outer_rows, preferred_element_type=jnp.float32
        ).astype(jnp.bfloat16),
        "dp",
        scatter_dimension=0,
        tiled=True,
    )
    grad_total = lax.psum(grad_shard, "sp").astype(jnp.float32)
    factor = 1.0 / math.sqrt(dp_count * seq_length)
    total_split = grad_total.reshape(grad_total.shape[0], head_total, 2, 2 * DQK)
    query_weight_grad = (
        total_split[:, :, 0].reshape(grad_total.shape[0], head_total * 2 * DQK) * factor
    )
    key_weight_grad = (
        total_split[:, :, 1].reshape(grad_total.shape[0], head_total * 2 * DQK) * factor
    )
    return (tokens_grad.astype(jnp.bfloat16)[None], values_grad, query_weight_grad, key_weight_grad)


LANES = 128
BF16 = jnp.bfloat16
F32 = jnp.float32
MIB = 1 << 20


def dot(a, b, dims=(((1,), (0,)), ((), ()))):
    return lax.dot_general(a, b, dims, preferred_element_type=F32)


def call(kernel, name, outs, scratch, in_specs, flops, limit, *args):
    moved = sum(math.prod(a.shape) * a.dtype.itemsize for a in (*args, *outs))
    vmem = pl.BlockSpec(memory_space=pltpu.VMEM)
    smem = pl.BlockSpec(memory_space=pltpu.SMEM)
    return pl.pallas_call(
        kernel,
        name=name,
        out_shape=outs,
        in_specs=[smem if k == "s" else vmem for k in in_specs],
        out_specs=[vmem] * len(outs),
        scratch_shapes=scratch,
        compiler_params=pltpu.CompilerParams(vmem_limit_bytes=limit * MIB),
        cost_estimate=pl.CostEstimate(flops=flops, bytes_accessed=moved, transcendentals=0),
    )(*args)


def shape(dims, dtype):
    return jax.ShapeDtypeStruct(dims, dtype)


def aligned(value, step):
    return pl.multiple_of(value, step)


def turn(tile, cosine, sine, sign):
    half = cosine.shape[0]
    parts = []
    for start in range(0, tile.shape[0], 2 * half):
        a = tile[start : start + half]
        b = tile[start + half : start + 2 * half]
        parts.append(a * cosine - b * (sign * sine))
        parts.append(b * cosine + a * (sign * sine))
    return jnp.concatenate(parts, axis=0)


def pack_kernel(heads, width, index, wq, wk, values, grads, w_out, *vg_outs):
    me = index[0]
    cols = heads * 2 * width
    vcols = vg_outs[0].shape[1] // 2
    mine = pl.ds(aligned(me * cols, LANES), cols)
    w_out[:, :cols] = wq[:, mine]
    w_out[:, cols:] = wk[:, mine]
    for k, out in enumerate(vg_outs):
        theirs = pl.ds(aligned((me ^ k) * vcols, LANES), vcols)
        out[:, :vcols] = values[:, theirs]
        out[:, vcols:] = grads[:, theirs]


def attention_kernel(
    heads, width, index, lambdas, cosine, sine,
    t_own, t_x, t_y, t_da, t_db,
    w0, w1, w2, w3, o0, o1, o2, o3,
    g0, g1, g2, g3,
    tok, wfull, back_t, back, vgrad,
    raw, rot_t, k_nat, v_nat, v_t, g_t, e_ref, mg_ref, sgm, acc,
):
    me, core, zed = index[0], index[1], index[2]
    rows = t_own.shape[0]
    half = rows // 2
    seq = tok.shape[0]
    cols = heads * 2 * width
    vcols = v_nat.shape[1]
    ve = vcols // heads
    blocks = seq // LANES
    wrows = w0.shape[0]
    inv_root = 1.0 / math.sqrt(width)
    for k, piece in ((0, t_own), (1, t_x), (2, t_y)):
        tok[pl.ds(aligned((me ^ k) * rows, half), rows), :] = piece[...]
    tok[pl.ds(aligned((me ^ 3) * rows, half), half), :] = t_da[...]
    tok[pl.ds(aligned((me ^ 3) * rows + half, half), half), :] = t_db[...]
    for k, (own, other) in enumerate(((w0, o0), (w1, o1), (w2, o2), (w3, o3))):
        base = (zed ^ k) * 2
        wfull[pl.ds(aligned((base + core) * wrows, wrows), wrows), :] = own[...]
        wfull[pl.ds(aligned((base + 1 - core) * wrows, wrows), wrows), :] = other[...]
    for n in range(0, 2 * cols, 256):
        raw[:, n : n + 256] = dot(tok[...], wfull[:, n : n + 256])
    for b in range(blocks):
        at = slice(b * LANES, (b + 1) * LANES)
        cos_b, sin_b = cosine[:, at], sine[:, at]
        for r in range(0, 2 * cols, LANES):
            turned = turn(jnp.transpose(raw[at, r : r + LANES]), cos_b, sin_b, 1.0)
            rot_t[r : r + LANES, at] = turned.astype(BF16)
            if r >= cols:
                k_nat[at, r - cols : r - cols + LANES] = jnp.transpose(turned).astype(BF16)
    stage = raw
    for k, piece in enumerate((g0, g1, g2, g3)):
        stage[pl.ds(aligned((me ^ k) * rows, half), rows), :] = piece[...].astype(F32)
    v_nat[...] = stage[:, :vcols].astype(BF16)
    for b in range(blocks):
        at = slice(b * LANES, (b + 1) * LANES)
        for r in range(0, vcols, LANES):
            v_t[r : r + LANES, at] = jnp.transpose(stage[at, r : r + LANES]).astype(BF16)
            g_t[r : r + LANES, at] = jnp.transpose(stage[at, vcols + r : vcols + r + LANES])

    scale2 = inv_root * math.log2(math.e)
    row_id = lax.broadcasted_iota(jnp.int32, (LANES, 2 * LANES), 0)
    col_id = lax.broadcasted_iota(jnp.int32, (LANES, 2 * LANES), 1)
    keep = row_id <= jnp.where(col_id < LANES, col_id, col_id - LANES)
    lane = lax.broadcasted_iota(jnp.int32, (LANES, LANES), 1)
    for h in range(heads):
        pair = (h // 2) * LANES
        odd = h % 2
        lam = lambdas[me * heads + h]
        zero = jnp.zeros((width, LANES), BF16)
        for i in reversed(range(blocks)):
            at = slice(i * LANES, (i + 1) * LANES)
            upto = (i + 1) * LANES
            q_t = rot_t[h * 2 * width : (h + 1) * 2 * width, at]
            diag = [
                jnp.concatenate([q_t[:width], zero], axis=1),
                jnp.concatenate([zero, q_t[width:]], axis=1),
            ]
            blank = jnp.zeros((2 * width, 2 * LANES), BF16)
            q_rhs = jnp.concatenate([blank, *diag] if odd else [*diag, blank], axis=0)
            top = jnp.full((8, 2 * LANES), -1e30, F32)
            for j in range(i + 1):
                ub = slice(j * LANES, (j + 1) * LANES)
                s = dot(k_nat[ub, pair : pair + LANES], q_rhs)
                if j == i:
                    s = jnp.where(keep, s, -1e30)
                e_ref[ub, :] = s
                top = jnp.maximum(top, jnp.max(s.reshape(LANES // 8, 8, 2 * LANES), axis=0))
            top = jnp.max(top, axis=0, keepdims=True) * scale2
            total = jnp.zeros((8, 2 * LANES), F32)
            for j in range(i + 1):
                ub = slice(j * LANES, (j + 1) * LANES)
                e = jnp.exp2(e_ref[ub, :] * scale2 - top)
                e_ref[ub, :] = e
                total = total + jnp.sum(e.reshape(LANES // 8, 8, 2 * LANES), axis=0)
            inv = 1.0 / jnp.sum(total, axis=0, keepdims=True)
            r1, r2 = inv[:, :LANES], inv[:, LANES:]
            a2 = lam * r2
            for j in range(i + 1):
                ub = slice(j * LANES, (j + 1) * LANES)
                mix = e_ref[ub, :LANES] * r1 - e_ref[ub, LANES:] * a2
                sgm[ub, 2 * LANES :] = mix.astype(BF16)
            ho = dot(v_t[h * ve : (h + 1) * ve, :upto], sgm[:upto, 2 * LANES :])
            g = g_t[h * ve : (h + 1) * ve, at]
            norm = lax.rsqrt(jnp.mean(ho * ho, axis=0, keepdims=True) + NORM_EPS)
            along = jnp.mean(g * ho, axis=0, keepdims=True)
            ob = (norm * g - norm * norm * norm * ho * along).astype(BF16)
            ob_blank = jnp.zeros_like(ob)
            ob_rhs = jnp.concatenate([ob_blank, ob] if odd else [ob, ob_blank], axis=0)
            d1 = jnp.zeros((8, LANES), F32)
            d2 = jnp.zeros((8, LANES), F32)
            for j in range(i + 1):
                ub = slice(j * LANES, (j + 1) * LANES)
                mg = dot(v_nat[ub, pair : pair + LANES], ob_rhs)
                mg_ref[ub, :] = mg
                d1 = d1 + jnp.sum((e_ref[ub, :LANES] * mg).reshape(LANES // 8, 8, LANES), axis=0)
                d2 = d2 + jnp.sum((e_ref[ub, LANES:] * mg).reshape(LANES // 8, 8, LANES), axis=0)
            d1 = jnp.sum(d1, axis=0, keepdims=True) * r1
            d2 = jnp.sum(d2, axis=0, keepdims=True) * r2
            f1 = r1 * inv_root
            f2 = a2 * (-inv_root)
            for j in range(i + 1):
                ub = slice(j * LANES, (j + 1) * LANES)
                mg = mg_ref[ub, :]
                sgm[ub, :LANES] = (e_ref[ub, :LANES] * f1 * (mg - d1)).astype(BF16)
                sgm[ub, LANES : 2 * LANES] = (e_ref[ub, LANES:] * f2 * (mg - d2)).astype(BF16)
            k_t = rot_t[cols + h * 2 * width : cols + (h + 1) * 2 * width, :upto]
            qt = dot(k_t, sgm[:upto, : 2 * LANES])
            qt = jnp.concatenate([qt[:width, :LANES], qt[width:, LANES:]], axis=0)
            qt = turn(qt, cosine[:, at], sine[:, at], -1.0)
            back_t[h * 2 * width : (h + 1) * 2 * width, at] = qt.astype(BF16)
            both = [q_t.astype(F32), ob.astype(F32)]
            nat = jnp.transpose(jnp.concatenate(both if odd else both[::-1], axis=0))
            k_at = 0 if odd else ve
            v_at = 2 * width if odd else 0
            rhs = jnp.concatenate(
                [
                    jnp.where((lane >= start) & (lane < start + size), nat, 0.0)
                    for start, size in ((k_at, width), (k_at + width, width), (v_at, ve))
                ],
                axis=0,
            ).astype(BF16)
            term = dot(sgm[:upto, :], rhs)
            if i == blocks - 1:
                acc[odd, :, :] = term
            else:
                acc[odd, :upto, :] += term
        k_at = 0 if odd else ve
        for b in range(blocks):
            at = slice(b * LANES, (b + 1) * LANES)
            kt = jnp.transpose(acc[odd, at, :])[k_at : k_at + 2 * width]
            kt = turn(kt, cosine[:, at], sine[:, at], -1.0)
            back_t[cols + h * 2 * width : cols + (h + 1) * 2 * width, at] = kt.astype(BF16)
            if odd:
                tile = jnp.where(lane < ve, acc[0, at, :], acc[1, at, :])
                vgrad[at, pair : pair + LANES] = tile.astype(BF16)
    for b in range(blocks):
        at = slice(b * LANES, (b + 1) * LANES)
        for r in range(0, 2 * cols, LANES):
            tile = back_t[r : r + LANES, at].astype(F32)
            back[at, r : r + LANES] = jnp.transpose(tile).astype(BF16)


def weight_grad_kernel(index, back_t, tok, keep, send):
    core = index[1]
    step = keep.shape[2]
    for z in range(keep.shape[0]):
        for part, out in ((core, keep), (1 - core, send)):
            at = pl.ds(aligned((2 * z + part) * step, LANES), step)
            out[z] = dot(back_t[...], tok[:, at]).astype(BF16)


def token_grad_kernel(index, back, wfull, send_x, send_y, keep_x, keep_y, own, order):
    me = index[0]
    seq = back.shape[0]
    rows = seq // 4
    half = rows // 2
    places = ((1, 0), (3, 0), (2, 1), (3, 1), (2, 0), (1, 1), (0, 0), (0, 1))
    for n, (k, part) in enumerate(places):
        at = pl.ds(aligned((me ^ k) * rows + part * half, half), half)
        order[n * half : (n + 1) * half, :] = back[at, :]
    for n in range(0, wfull.shape[0], 256):
        at = slice(n, n + 256)
        part = dot(order[...], wfull[at, :], (((1,), (1,)), ((), ())))
        send_x[:, at] = part[: 2 * half].astype(BF16)
        send_y[:, at] = part[2 * half : 4 * half].astype(BF16)
        keep_y[:, at] = part[4 * half : 5 * half]
        keep_x[:, at] = part[5 * half : 6 * half]
        own[:, at] = part[6 * half :]


def pair_sum_kernel(index, keep, got, own, s1, s2, s3):
    zed = index[2]
    for k, out in enumerate((own, s1, s2, s3)):
        at = zed ^ k
        out[...] = (keep[at].astype(F32) + got[at].astype(F32)).astype(out.dtype)


def depth_sum_kernel(own, r1, r2, r3, out):
    total = own[...] + r1[...].astype(F32) + r2[...].astype(F32) + r3[...].astype(F32)
    out[...] = jnp.transpose(total).astype(BF16)


def place_kernel(factor, cols, index, own, got_x, got_y, da, db, wq, wk):
    me = index[0]
    half = da.shape[0]
    everything = slice(None)
    for k, piece, at in (
        (0, own, everything),
        (1, got_x, everything),
        (2, got_y, everything),
        (3, da, slice(0, half)),
        (3, db, slice(half, 2 * half)),
    ):
        theirs = pl.ds(aligned((me ^ k) * cols, LANES), cols)
        wq[at, theirs] = piece[:, :cols].astype(F32) * factor
        wk[at, theirs] = piece[:, cols:].astype(F32) * factor


def values_kernel(index, vgrad, r1, r2, r3, out):
    me = index[0]
    rows = r1.shape[0]
    cols = r1.shape[1]
    mine = pl.ds(aligned(me * rows, rows // 2), rows)
    out[:, pl.ds(aligned(me * cols, LANES), cols)] = vgrad[mine, :]
    for k, piece in ((1, r1), (2, r2), (3, r3)):
        out[:, pl.ds(aligned((me ^ k) * cols, LANES), cols)] = piece[...]


def flip(value, axis, mask):
    count = lax.axis_size(axis)
    return lax.ppermute(value, axis, [(i, i ^ mask) for i in range(count)])


def quarter_body(tokens, query_weight, key_weight, values, lambdas, out_grad):
    sp_count = lax.axis_size("sp")
    dp_count = lax.axis_size("dp")
    rows, depth = tokens.shape[1:]
    head_total = lambdas.shape[0]
    heads = head_total // sp_count
    seq = rows * sp_count
    cols = heads * 2 * DQK
    vcols = values.shape[2] // sp_count
    wrows = query_weight.shape[0]
    half = rows // 2
    me = lax.axis_index("sp")
    line = lax.axis_index("dp")
    index = jnp.stack([me, line % 2, line // 2]).astype(jnp.int32)
    cosine, sine = rotation_tables(jnp.arange(seq, dtype=jnp.int32), DQK)
    own_tok = tokens[0]
    tok_x = flip(own_tok, "sp", 1)
    tok_y = flip(own_tok, "sp", 2)
    w_own, *vg = call(
        functools.partial(pack_kernel, heads, DQK),
        "pack",
        [shape((wrows, 2 * cols), BF16)] + [shape((rows, 2 * vcols), BF16)] * 4,
        [],
        "svvvv",
        1 << 20,
        16,
        index, query_weight, key_weight, values[0], out_grad[0],
    )
    w_line = [w_own] + [flip(w_own, "dp", 2 * k) for k in (1, 2, 3)]
    vg = [vg[0]] + [flip(vg[k], "sp", k) for k in (1, 2, 3)]
    w_other = [flip(w, "dp", 1) for w in w_line]
    tok_da = flip(tok_x[:half], "sp", 2)
    tok_db = flip(tok_y[half:], "sp", 1)
    pair_cols = heads * DQK * 2
    tok, wfull, back_t, back, vgrad = call(
        functools.partial(attention_kernel, heads, DQK),
        "attention",
        [
            shape((seq, depth), BF16),
            shape((depth, 2 * cols), BF16),
            shape((2 * cols, seq), BF16),
            shape((seq, 2 * cols), BF16),
            shape((seq, vcols), BF16),
        ],
        [
            pltpu.VMEM((seq, 2 * max(cols, vcols)), F32),
            pltpu.VMEM((2 * cols, seq), BF16),
            pltpu.VMEM((seq, pair_cols), BF16),
            pltpu.VMEM((seq, vcols), BF16),
            pltpu.VMEM((vcols, seq), BF16),
            pltpu.VMEM((vcols, seq), F32),
            pltpu.VMEM((seq, 2 * LANES), F32),
            pltpu.VMEM((seq, LANES), F32),
            pltpu.VMEM((seq, 3 * LANES), BF16),
            pltpu.VMEM((2, seq, LANES), F32),
        ],
        "ss" + "v" * 19,
        10 * seq * depth * cols,
        40,
        index, lambdas, cosine.T, sine.T,
        own_tok, tok_x, tok_y, tok_da, tok_db,
        *w_line, *w_other, *vg,
    )
    chips = dp_count // 2
    keep_w, send_w = call(
        weight_grad_kernel,
        "weight_grad",
        [shape((chips, 2 * cols, wrows), BF16)] * 2,
        [],
        "svv",
        4 * seq * depth * cols,
        24,
        index, back_t, tok,
    )
    got_w = flip(send_w, "dp", 1)
    send_x, send_y, keep_x, keep_y, own_t = call(
        token_grad_kernel,
        "token_grad",
        [shape((rows, depth), BF16)] * 2
        + [shape((half, depth), F32)] * 2
        + [shape((rows, depth), F32)],
        [pltpu.VMEM((seq, 2 * cols), BF16)],
        "svv",
        4 * seq * depth * cols,
        24,
        index, back, wfull,
    )
    got_x = flip(send_x, "sp", 1)
    got_y = flip(send_y, "sp", 2)
    own_w, *sums = call(
        pair_sum_kernel,
        "pair_sum",
        [shape((2 * cols, wrows), F32)] + [shape((2 * cols, wrows), BF16)] * 3,
        [],
        "svv",
        1 << 20,
        16,
        index, keep_w, got_w,
    )
    got_line = [flip(w, "dp", 2 * k) for k, w in zip((1, 2, 3), sums)]
    v_out = [
        flip(lax.dynamic_slice_in_dim(vgrad, (me ^ k) * rows, rows, 0), "sp", k) for k in (1, 2, 3)
    ]
    pass_y = (keep_y + got_x[half:].astype(F32)).astype(BF16)
    pass_x = (keep_x + got_y[half:].astype(F32)).astype(BF16)
    last_y = flip(pass_y, "sp", 2)
    last_x = flip(pass_x, "sp", 1)
    near = jnp.concatenate([got_x[:half], got_y[:half]], axis=0).astype(F32)
    far = jnp.concatenate([last_y, last_x], axis=0).astype(F32)
    tokens_grad = (own_t + near + far).astype(BF16)
    (values_grad,) = call(
        values_kernel,
        "values",
        [shape((rows, vcols * sp_count), BF16)],
        [],
        "svvvv",
        1 << 18,
        8,
        index, vgrad, *v_out,
    )
    (w_sum,) = call(
        depth_sum_kernel,
        "depth_sum",
        [shape((wrows, 2 * cols), BF16)],
        [],
        "vvvv",
        1 << 18,
        8,
        own_w, *got_line,
    )
    w_x = flip(w_sum, "sp", 1)
    w_y = flip(w_sum, "sp", 2)
    w_da = flip(w_x[: wrows // 2], "sp", 2)
    w_db = flip(w_y[wrows // 2 :], "sp", 1)
    factor = 1.0 / math.sqrt(dp_count * seq)
    query_weight_grad, key_weight_grad = call(
        functools.partial(place_kernel, factor, cols),
        "place",
        [shape((wrows, cols * sp_count), F32)] * 2,
        [],
        "svvvvv",
        1 << 18,
        8,
        index, w_sum, w_x, w_y, w_da, w_db,
    )
    return (tokens_grad[None], values_grad[None], query_weight_grad, key_weight_grad)


def solution(mesh):
    in_specs = (
        P("dp", "sp", None),
        P("dp", None),
        P("dp", None),
        P("dp", "sp", None),
        P(),
        P("dp", "sp", None),
    )
    out_specs = (P("dp", "sp", None), P("dp", "sp", None), P("dp", None), P("dp", None))
    quarter = mesh.shape["sp"] == 4 and mesh.shape["dp"] == 8
    body = quarter_body if quarter else general_body
    return jax.shard_map(body, mesh=mesh, in_specs=in_specs, out_specs=out_specs, check_vma=False)
```
